512 devices in a mesh: fs: 16 (over y, x), tp: 32 (over z, core).
Axes of the slice: x: 4, y: 4, z: 16, core: 2. Of those that a mesh axis runs over, the one named last changes fastest.
Arguments:
- inputs: bfloat16 [32, 320, 2048], P('tp'), may hold values from -6 to 6
- cotangent: bfloat16 [32, 320, 2048], P('tp'), may hold values from -8 to 8
- gate_weight: bfloat16 [2048, 5632], P('tp', 'fs'), may hold values from -0.125 to 0.125
- up_weight: bfloat16 [2048, 5632], P('tp', 'fs'), may hold values from -0.125 to 0.125
- down_weight: bfloat16 [5632, 2048], P('fs', 'tp'), may hold values from -0.078125 to 0.078125
Outputs:
- input_grad: bfloat16 [32, 320, 2048], P('tp')
- down_grad: float32 [5632, 2048], P('fs', 'tp')
The draws below stay inside these ranges and needn't reach their ends.
All inputs are finite; a program needn't handle non-finite values.
Results may differ from the reference program's by a relative error of at most 0.023.
Values may be sent and summed in bfloat16 or wider, within the bound.
No kernel may reach another device: no remote copies, remote signals or barrier semaphores. Data moves between devices by JAX's collectives and lax.ppermute only.
A program may use at most 64 MiB of HBM per device.

```python
import jax
import jax.numpy as jnp
from jax import lax

D = 2048
FF = 5632
TOK_DEV = 320
SPANS = 32
N_FS = 16


def spiked(array, key, source, target, shards_of, factor):
    def block_of(position):
        return (jnp.arange(array.shape[position]) // (array.shape[position] // shards_of)).reshape((-1,) + (1,) * (array.ndim - 1 - position))

    first = jax.random.permutation(key, shards_of)[block_of(target)]
    other_side = (block_of(target) + shards_of // 2) % shards_of
    return jnp.where((block_of(source) == first) | (block_of(source) == other_side), factor * array, array)


def levels(rng, shape, cuts, low, high):
    loudness, own = 1.0, jax.random.fold_in(rng, 6)
    for position, blocks in cuts:
        heights = jnp.exp(jax.random.uniform(jax.random.fold_in(own, position), (blocks,), jnp.float32, low / len(cuts), high / len(cuts)))
        loudness = loudness * jnp.repeat(heights, shape[position] // blocks).reshape([-1 if axis == position else 1 for axis in range(len(shape))])
    return loudness


def centred(stream_key, extent, scale, limit, cuts=(), dtype=jnp.bfloat16):
    values = scale * jax.random.normal(stream_key, extent, jnp.float32)
    if cuts:
        values = values * levels(stream_key, extent, cuts, -0.22, 0.18)
    return jnp.clip(values, -limit, limit).astype(dtype)


def noise_with(own_key, extent, scale, limit, cuts, heavy, kind=jnp.bfloat16):
    array = scale * jax.random.normal(own_key, extent, jnp.float32)
    if cuts:
        array = array * levels(own_key, extent, cuts, -0.22, 0.18)
    return jnp.clip(spiked(array, jax.random.fold_in(own_key, 3), *heavy), -limit, limit).astype(kind)


def setup_inputs(seed: int = 0) -> dict:
    splits = jax.random.split(jax.random.key(seed), 6)
    inputs = centred(splits[0], (SPANS, TOK_DEV, D), 1.0, 6.0, ((0, 32),))
    cotangent = noise_with(splits[1], (SPANS, TOK_DEV, D), 1.0, 8.0, ((0, 32),), (0, 2, 32, 2.75))
    gate_weight = centred(splits[2], (D, FF), D ** -0.5, 0.125, ((0, 32), (1, 16)))
    up_weight = centred(splits[3], (D, FF), D ** -0.5, 0.125, ((0, 32), (1, 16)))
    down_weight = centred(splits[4], (FF, D), FF ** -0.5, 0.078125, ((0, 16), (1, 32)))
    return {"inputs": inputs, "cotangent": cotangent, "gate_weight": gate_weight, "up_weight": up_weight, "down_weight": down_weight}


def reference(inputs, cotangent, gate_weight, up_weight, down_weight):
    rows_in = inputs.reshape(-1, D)
    rows_grad = cotangent.reshape(-1, D)
    gate_pre = jnp.dot(rows_in, gate_weight, preferred_element_type=jnp.float32)
    up_pre = jnp.dot(rows_in, up_weight, preferred_element_type=jnp.float32)
    sig = jax.nn.sigmoid(gate_pre)
    hidden = (gate_pre * sig * up_pre).astype(jnp.bfloat16)
    down_grad = jnp.dot(hidden.T, rows_grad, preferred_element_type=jnp.float32)
    hidden_grad = jnp.dot(rows_grad, down_weight.T, preferred_element_type=jnp.float32)
    gate_grad = (hidden_grad * up_pre * sig * (1.0 + gate_pre * (1.0 - sig))).astype(jnp.bfloat16)
    up_grad = (hidden_grad * gate_pre * sig).astype(jnp.bfloat16)
    width = FF // N_FS
    total_rows = rows_in.shape[0]
    gate_blocks = gate_weight.reshape(D, N_FS, width).transpose(1, 0, 2)
    up_blocks = up_weight.reshape(D, N_FS, width).transpose(1, 0, 2)
    gate_cols = gate_grad.reshape(total_rows, N_FS, width).transpose(1, 0, 2)
    up_cols = up_grad.reshape(total_rows, N_FS, width).transpose(1, 0, 2)

    def add_block(total, pieces):
        g_weight, u_weight, g_cols, u_cols = pieces
        term = jnp.dot(g_cols, g_weight.T, preferred_element_type=jnp.float32)
        term = term + jnp.dot(u_cols, u_weight.T, preferred_element_type=jnp.float32)
        return total + term.astype(jnp.bfloat16).astype(jnp.float32), None

    start_total = jnp.zeros((total_rows, D), jnp.float32)
    total, unused = lax.scan(add_block, start_total, (gate_blocks, up_blocks, gate_cols, up_cols))
    input_grad = total.astype(jnp.bfloat16).reshape(inputs.shape)
    return input_grad, down_grad
```

```python
import jax
import jax.numpy as jnp
from jax import lax
from jax.sharding import Mesh
from jax.sharding import PartitionSpec as P

TP = ("zh", "zl", "c")
WEIGHT_SCALE = 2.0**18


def contract_hidden(left, right):
    return lax.dot_general(
        left, right, (((1,), (1,)), ((), ())), preferred_element_type=jnp.float32
    )


def contract_tokens(left, right):
    return lax.dot_general(
        left, right, (((0,), (0,)), ((), ())), preferred_element_type=jnp.float32
    )


def per_device(inputs, cotangent, gate_weight, up_weight, down_weight):
    rows_in = inputs[0]
    rows_grad = cotangent[0]
    tokens, width = rows_in.shape
    hid = gate_weight.shape[1]
    both = jnp.concatenate((gate_weight, up_weight, down_weight.T), axis=1)
    both = (both.astype(jnp.float32) * WEIGHT_SCALE).astype(jnp.float16)
    full = lax.all_gather(both, TP, axis=0, tiled=True)
    full = (full.astype(jnp.float32) * (1.0 / WEIGHT_SCALE)).astype(jnp.bfloat16)
    gate_full = full[:, :hid]
    up_full = full[:, hid : 2 * hid]
    down_tall = full[:, 2 * hid :]
    gate_pre = jnp.dot(rows_in, gate_full, preferred_element_type=jnp.float32)
    up_pre = jnp.dot(rows_in, up_full, preferred_element_type=jnp.float32)
    sig = jax.nn.sigmoid(gate_pre)
    hidden = (gate_pre * sig * up_pre).astype(jnp.bfloat16)
    hidden_grad = jnp.dot(rows_grad, down_tall, preferred_element_type=jnp.float32)
    gate_grad = (hidden_grad * up_pre * sig * (1.0 + gate_pre * (1.0 - sig))).astype(jnp.bfloat16)
    up_grad = (hidden_grad * gate_pre * sig).astype(jnp.bfloat16)

    term = (contract_hidden(gate_grad, gate_full) + contract_hidden(up_grad, up_full)).astype(
        jnp.bfloat16
    )
    n_fs = lax.axis_size("fs")
    pieces = term.reshape(tokens, n_fs, width // n_fs).transpose(1, 0, 2)
    parts = lax.all_to_all(pieces, "fs", 0, 0, tiled=True)
    own = jnp.sum(parts.astype(jnp.float32), axis=0).astype(jnp.bfloat16)

    zh, zl, c = (lax.axis_size(a) for a in TP)
    partial = contract_tokens(rows_grad, hidden)
    partial = partial.reshape(zh, zl, c, width // (zh * zl * c), hid)
    me = lax.axis_index("c")
    mine = lax.dynamic_index_in_dim(partial, me, 2, keepdims=False)
    other = lax.dynamic_index_in_dim(partial, 1 - me, 2, keepdims=False).astype(jnp.bfloat16)
    got = lax.ppermute(other, "c", [(0, 1), (1, 0)])
    pair = (mine + got.astype(jnp.float32)).astype(jnp.bfloat16)
    near = lax.all_to_all(pair, "zl", 1, 1, tiled=True)
    near = jnp.sum(near.astype(jnp.float32), axis=1).astype(jnp.bfloat16)
    far = lax.all_to_all(near, "zh", 0, 0, tiled=True)
    down_grad = jnp.sum(far.astype(jnp.float32), axis=0).T

    copies = jnp.broadcast_to(own, (n_fs, *own.shape))
    whole = lax.all_to_all(copies, "fs", 0, 0, tiled=True)
    input_grad = whole.transpose(1, 0, 2).reshape(1, tokens, width)
    return (input_grad, down_grad)


def solution(mesh):
    finer = Mesh(mesh.devices.reshape(mesh.shape["fs"], 4, 4, 2), ("fs", "zh", "zl", "c"))
    return jax.shard_map(
        per_device,
        mesh=finer,
        in_specs=(P(TP, None, None), P(TP, None, None), P(TP, "fs"), P(TP, "fs"), P("fs", TP)),
        out_specs=(P(TP, None, None), P("fs", TP)),
        check_vma=False,
    )
```

```python
import jax
import jax.numpy as jnp
from jax import lax
from jax.experimental import pallas as pl
from jax.experimental.pallas import tpu as pltpu
from jax.sharding import Mesh
from jax.sharding import PartitionSpec as P

TP = ("zh", "zl", "c")
WEIGHT_SCALE = 2.0**18


def contract_hidden(left, right):
    return lax.dot_general(
        left, right, (((1,), (1,)), ((), ())), preferred_element_type=jnp.float32
    )


def down_kernel(where, cot, hidden, mine, other):
    core, zl = where[0], where[1]
    hid = hidden[...]
    for z in range(16):
        block = lax.dot_general(
            cot[:, z * 128 : (z + 1) * 128],
            hid,
            (((0,), (0,)), ((), ())),
            preferred_element_type=jnp.float32,
        )
        slot = jnp.bitwise_and(z % 4 - zl + 4, 3)
        top, bottom = block[:64], block[64:]
        mine[slot, z // 4] = jnp.where(core == 0, top, bottom)
        other[slot, z // 4] = jnp.where(core == 0, bottom, top).astype(jnp.bfloat16)


def down_partial(where, cot, hidden):
    tokens, width = cot.shape
    hid = hidden.shape[1]
    shape = (4, 4, 64, hid)
    return pl.pallas_call(
        down_kernel,
        out_shape=(
            jax.ShapeDtypeStruct(shape, jnp.float32),
            jax.ShapeDtypeStruct(shape, jnp.bfloat16),
        ),
        in_specs=[
            pl.BlockSpec(memory_space=pltpu.SMEM),
            pl.BlockSpec(memory_space=pltpu.VMEM),
            pl.BlockSpec(memory_space=pltpu.VMEM),
        ],
        out_specs=(
            pl.BlockSpec(memory_space=pltpu.VMEM),
            pl.BlockSpec(memory_space=pltpu.VMEM),
        ),
        cost_estimate=pl.CostEstimate(
            flops=2 * tokens * width * hid, bytes_accessed=6 * width * hid, transcendentals=0
        ),
        compiler_params=pltpu.CompilerParams(vmem_limit_bytes=12 << 20),
        name="down_partial",
    )(where, cot, hidden)


def join_kernel(pieces, out):
    for j in range(16):
        out[:, j * 128 : (j + 1) * 128] = pieces[j]


def joined(pieces):
    n, tokens, cols = pieces.shape
    rows = 80
    return pl.pallas_call(
        join_kernel,
        grid=(tokens // rows,),
        out_shape=jax.ShapeDtypeStruct((tokens, n * cols), pieces.dtype),
        in_specs=[pl.BlockSpec((n, rows, cols), lambda i: (0, i, 0))],
        out_specs=pl.BlockSpec((rows, n * cols), lambda i: (i, 0)),
        cost_estimate=pl.CostEstimate(
            flops=tokens * n * cols, bytes_accessed=4 * tokens * n * cols, transcendentals=0
        ),
        compiler_params=pltpu.CompilerParams(vmem_limit_bytes=4 << 20),
        name="join_pieces",
    )(pieces)


def turn(step):
    return [(i, (i + step) % 4) for i in range(4)]


def per_device(inputs, cotangent, gate_weight, up_weight, down_weight):
    rows_in = inputs[0]
    rows_grad = cotangent[0]
    tokens, width = rows_in.shape
    hid = gate_weight.shape[1]
    both = jnp.concatenate((gate_weight, up_weight, down_weight.T), axis=1)
    both = (both.astype(jnp.float32) * WEIGHT_SCALE).astype(jnp.float16)
    full = lax.all_gather(both, TP, axis=0, tiled=True)
    full = (full.astype(jnp.float32) * (1.0 / WEIGHT_SCALE)).astype(jnp.bfloat16)
    gate_full = full[:, :hid]
    up_full = full[:, hid : 2 * hid]
    down_tall = full[:, 2 * hid :]
    gate_pre = jnp.dot(rows_in, gate_full, preferred_element_type=jnp.float32)
    up_pre = jnp.dot(rows_in, up_full, preferred_element_type=jnp.float32)
    sig = jax.nn.sigmoid(gate_pre)
    hidden = (gate_pre * sig * up_pre).astype(jnp.bfloat16)
    hidden_grad = jnp.dot(rows_grad, down_tall, preferred_element_type=jnp.float32)
    gate_grad = (hidden_grad * up_pre * sig * (1.0 + gate_pre * (1.0 - sig))).astype(jnp.bfloat16)
    up_grad = (hidden_grad * gate_pre * sig).astype(jnp.bfloat16)

    where = jnp.stack((lax.axis_index("c"), lax.axis_index("zl"))).astype(jnp.int32)
    mine, other = down_partial(where, rows_grad, hidden)
    got = lax.ppermute(other, "c", [(0, 1), (1, 0)])

    term = (contract_hidden(gate_grad, gate_full) + contract_hidden(up_grad, up_full)).astype(
        jnp.bfloat16
    )
    n_fs = lax.axis_size("fs")
    pieces = term.reshape(tokens, n_fs, width // n_fs).transpose(1, 0, 2)
    parts = lax.all_to_all(pieces, "fs", 0, 0, tiled=True)

    pair = [(mine[k] + got[k].astype(jnp.float32)).astype(jnp.bfloat16) for k in range(4)]
    near = pair[0].astype(jnp.float32)
    for k in (1, 3, 2):
        near = near + lax.ppermute(pair[k], "zl", turn(k)).astype(jnp.float32)
    near = near.astype(jnp.bfloat16)
    parts, near = lax.optimization_barrier((parts, near))
    own = jnp.sum(parts.astype(jnp.float32), axis=0).astype(jnp.bfloat16)
    zh = lax.axis_index("zh")
    chunk = [lax.dynamic_index_in_dim(near, (zh + k) % 4, 0, keepdims=False) for k in range(4)]
    far = chunk[0].astype(jnp.float32)
    for k in (1, 3, 2):
        far = far + lax.ppermute(chunk[k], "zh", turn(k)).astype(jnp.float32)
    down_grad = far.T

    copies = jnp.broadcast_to(own, (n_fs, *own.shape))
    whole = lax.all_to_all(copies, "fs", 0, 0, tiled=True)
    input_grad = joined(whole)[None]
    return (input_grad, down_grad)


def solution(mesh):
    finer = Mesh(mesh.devices.reshape(mesh.shape["fs"], 4, 4, 2), ("fs", "zh", "zl", "c"))
    return jax.shard_map(
        per_device,
        mesh=finer,
        in_specs=(P(TP, None, None), P(TP, None, None), P(TP, "fs"), P(TP, "fs"), P("fs", TP)),
        out_specs=(P(TP, None, None), P("fs", TP)),
        check_vma=False,
    )
```
